32 devices in a mesh: sp: 8 (over z, core), tp: 4 (over y, x).
Axes of the slice: x: 2, y: 2, z: 4, core: 2. Of those that a mesh axis runs over, the one named last changes fastest.
Arguments:
- residual: bfloat16 [1024, 2048], P('sp', 'tp'), may hold values from -48 to 48
- glu_value: bfloat16 [1024, 2048], P('sp', 'tp'), may hold values from -48 to 48
- glu_gate: bfloat16 [1024, 2048], P('sp', 'tp'), may hold values from -6 to 6
- conv_weight: bfloat16 [31, 2048], P(None, 'tp'), may hold values from -1 to 1
- conv_bias: float32 [2048], P('tp'), may hold values from -3 to 3
- ln_gain: float32 [2048], P('tp'), may hold values from 0.1 to 1.9
- ln_bias: float32 [2048], P('tp'), may hold values from -3 to 3
- out_weight: bfloat16 [2048, 2048], P(None, 'tp'), may hold values from -0.125 to 0.125
- norm_gain: float32 [2048], P('tp'), may hold values from 0.1 to 1.9
- route_ids: int32 [1024, 2], P('sp'), may hold values from 0 to 7, all different within a row; in each aligned block of 128 rows (0 to 127, 128 to 255, ...) at most 64 rows name the same one
- route_weight: float32 [1024, 2], P('sp'), may hold values from 0.1 to 1
- expert_gate: bfloat16 [8, 2048, 4096], P('sp', None, 'tp'), may hold values from -0.125 to 0.125
- expert_up: bfloat16 [8, 2048, 4096], P('sp', None, 'tp'), may hold values from -0.125 to 0.125
- expert_down: bfloat16 [8, 4096, 2048], P('sp', 'tp'), may hold values from -0.09375 to 0.09375
Outputs:
- layer_out: bfloat16 [1024, 2048], P('sp', 'tp')
The draws below stay inside these ranges and needn't reach their ends.
Inputs may be any that keep to these rules, and one draw needn't show every extreme that they name: `route_ids`: within the 128 rows of one index of sp, no expert is named more than 64 times, and in some such rows one expert is named exactly 64 times.
All inputs are finite; a program needn't handle non-finite values.
Results may differ from the reference program's by a relative error of at most 0.006.
Values may be sent and summed in bfloat16 or wider, within the bound.
A program may use at most 64 MiB of HBM per device.

```python
import math
import jax
import jax.numpy as jnp
import numpy as np
from jax import lax

D = 2048
FF = 4096
KERNEL = 31
TOPK = 2
ROWS = 128
TOKENS = 1024
EXPERTS = 8
CAP = 64
N_SP = 8
N_TP = 4


def rising_field(key, low, high):
    ramp = jnp.exp(jnp.linspace(math.log(low), math.log(high), D)).astype(jnp.float32)
    base = jnp.clip(jax.random.normal(key, (TOKENS, D), jnp.float32), -6.0, 6.0)
    return base * ramp


def draw_residual(key, part):
    return rising_field(jax.random.fold_in(key, 11), 0.5, 2.0).astype(jnp.bfloat16)


def draw_glu_value(key, part):
    return rising_field(jax.random.fold_in(key, 23), 0.5, 2.0).astype(jnp.bfloat16)


def levels(stream_key, dims, shards, least, largest):
    def one(position, parts):
        heights = jax.random.uniform(jax.random.fold_in(jax.random.fold_in(stream_key, 6), position), (parts,), jnp.float32, least / len(shards), largest / len(shards))
        return jnp.repeat(jnp.exp(heights), dims[position] // parts).reshape((-1,) + (1,) * (len(dims) - position - 1))

    loudness = one(*shards[0])
    for cut in shards[1:]:
        loudness = loudness * one(*cut)
    return loudness


def routed_block(rng, own, number, rows, count, top, most, skew):
    order = jax.random.permutation(rng, count)
    heavy_load, ordinary = portions_of(count, rows * top, most, skew, True), portions_of(count, rows * top, most, skew, False)
    places = jnp.arange(count)

    def named(lengths, turn):
        used = int((lengths > 0).sum())
        fixed = max(1, used // 4)
        moved = fixed + (places - fixed + turn * (used - fixed)) % max(1, count - fixed)
        return jnp.zeros((count,), jnp.int32).at[order[jnp.where(places < fixed, places, moved)]].set(jnp.asarray(lengths, jnp.int32))

    lengths = jnp.where(number % 4 == 0, named(heavy_load, number // 4), named(ordinary, number - number // 4 - 1))
    mixed = jax.random.permutation(jax.random.fold_in(own, 3), count)
    giver, sink = mixed[0:count // 2 * 2:2], mixed[1:count // 2 * 2:2]
    slack = jnp.minimum(lengths[giver] - 1, most - lengths[sink]) // 2
    slack = jnp.where((giver == order[0]) | (sink == order[0]) | (lengths[sink] == 0), 0, jnp.maximum(slack, 0))
    moved = jax.random.randint(jax.random.fold_in(own, 4), (count // 2,), 0, 1 << 20) % (slack + 1)
    lengths = lengths.at[giver].add(-moved).at[sink].add(moved)
    items = jnp.searchsorted(jnp.cumsum(lengths), jnp.arange(rows * top), side="right").astype(jnp.int32)
    table = items.reshape(top, rows).T
    table = table[jax.random.permutation(jax.random.fold_in(own, 1), rows)]
    turn = jax.random.randint(jax.random.fold_in(own, 2), (rows, 1), 0, top)
    return jnp.take_along_axis(table, (jnp.arange(top)[None, :] + turn) % top, axis=1)


def portions_of(count, total, bound, lean, full):
    loads = [(1 << 20) // math.isqrt(rank ** lean) + 1 for rank in range(1, count + 1)]
    largest = bound if full else min(bound, max(-(-total // count), total * loads[0] // sum(loads)))
    least = 1 if total - largest >= count - 1 else 0
    counts, spare = [largest] + [least] * (count - 1), total - largest - least * (count - 1)
    while spare > 0:
        candidates = [i for i in range(1, count) if counts[i] < largest] or [i for i in range(1, count) if counts[i] < bound]
        whole, left = sum([loads[i] for i in candidates]), spare
        for i in candidates:
            extra = min(bound - counts[i], max(1, left * loads[i] // whole), spare)
            counts[i] = counts[i] + extra
            spare = spare - extra
    return np.array(counts)


def gaussian(rng, shape, spread, limit, cuts=(), kind=jnp.bfloat16):
    drawn = spread * jax.random.normal(rng, shape, jnp.float32)
    if cuts:
        drawn = drawn * levels(rng, shape, cuts, -0.22, 0.18)
    return jnp.clip(drawn, -limit, limit).astype(kind)


def setup_inputs(seed: int = 0) -> dict:
    arg_keys = jax.random.split(jax.random.key(seed), 15)
    residual = draw_residual(jax.random.fold_in(arg_keys[14], 71), 0)
    glu_value = draw_glu_value(jax.random.fold_in(arg_keys[14], 71), 0)
    glu_gate = gaussian(arg_keys[2], (TOKENS, D), 1.0, 6.0, ((0, 8), (1, 4)))
    conv_weight = gaussian(arg_keys[3], (KERNEL, D), KERNEL ** -0.5, 1.0, ((1, 4),))
    conv_bias = gaussian(arg_keys[4], (D,), 0.5, 3.0, ((0, 4),), jnp.float32)
    ln_gain = jnp.clip(1.0 + 0.18 * jax.random.normal(arg_keys[5], (D,), jnp.float32), 0.1, 1.9)
    ln_bias = gaussian(arg_keys[6], (D,), 0.5, 3.0, ((0, 4),), jnp.float32)
    out_weight = gaussian(arg_keys[7], (D, D), D ** -0.5, 0.125, ((1, 4),))
    norm_gain = jnp.clip(1.0 + 0.18 * jax.random.normal(arg_keys[8], (D,), jnp.float32), 0.1, 1.9)
    route_ids_keys = jax.random.split(jax.random.fold_in(arg_keys[9], 1), TOKENS // ROWS)
    route_ids_turns = jax.random.permutation(jax.random.fold_in(arg_keys[9], 3), TOKENS // ROWS)
    route_ids = jax.vmap(lambda own, number: routed_block(jax.random.fold_in(arg_keys[9], 2), own, number, ROWS, EXPERTS, TOPK, CAP, 2))(route_ids_keys, route_ids_turns).reshape((TOKENS, TOPK))
    route_weight = jnp.clip(jnp.exp(math.log(1.0) - 2.3025851 * jax.random.uniform(arg_keys[10], (TOKENS, TOPK), jnp.float32) ** levels(arg_keys[10], (TOKENS, TOPK), ((0, 8),), -0.2, 0.2)), 0.1, 1.0)
    expert_gate = gaussian(arg_keys[11], (EXPERTS, D, FF), D ** -0.5, 0.125, ((0, 8), (2, 4)))
    expert_up = gaussian(arg_keys[12], (EXPERTS, D, FF), D ** -0.5, 0.125, ((0, 8), (2, 4)))
    expert_down = gaussian(arg_keys[13], (EXPERTS, FF, D), FF ** -0.5, 0.09375, ((0, 8), (1, 4)))
    return dict(residual=residual, glu_value=glu_value, glu_gate=glu_gate, conv_weight=conv_weight, conv_bias=conv_bias, ln_gain=ln_gain, ln_bias=ln_bias, out_weight=out_weight, norm_gain=norm_gain, route_ids=route_ids, route_weight=route_weight, expert_gate=expert_gate, expert_up=expert_up, expert_down=expert_down)


def reference(residual, glu_value, glu_gate, conv_weight, conv_bias, ln_gain, ln_bias, out_weight, norm_gain, route_ids, route_weight, expert_gate, expert_up, expert_down):
    gated = (glu_value.astype(jnp.float32) * jax.nn.sigmoid(glu_gate.astype(jnp.float32))).astype(jnp.bfloat16)
    reach = KERNEL // 2
    padded = jnp.pad(gated.astype(jnp.float32), ((reach, reach), (0, 0)))
    taps = conv_weight.astype(jnp.float32)
    conv = jnp.zeros(gated.shape, jnp.float32) + conv_bias
    for tap in range(KERNEL):
        conv = conv + padded[tap:tap + TOKENS] * taps[tap]
    mean = lax.optimization_barrier(jnp.mean(conv, axis=1, keepdims=True))
    var = lax.optimization_barrier(jnp.mean(conv * conv, axis=1, keepdims=True)) - mean * mean
    act = jax.nn.silu((conv - mean) * lax.rsqrt(var + 1e-05) * ln_gain + ln_bias).astype(jnp.bfloat16)
    mixed = residual.astype(jnp.float32) + jnp.dot(act, out_weight, preferred_element_type=jnp.float32)
    squares = lax.optimization_barrier(jnp.mean(mixed * mixed, axis=1, keepdims=True))
    normed = (mixed * lax.rsqrt(squares + 1e-06) * norm_gain).astype(jnp.bfloat16)
    flat = route_ids.reshape(-1)
    owner = (jnp.arange(TOKENS * TOPK, dtype=jnp.int32) // TOPK).astype(jnp.int32)
    weights = route_weight.reshape(-1)
    slots = N_SP * CAP
    slot_index = jnp.arange(slots, dtype=jnp.int32)
    block = FF // N_TP

    def per_expert(total, expert):
        chosen = flat == expert
        picks = jnp.nonzero(chosen, size=slots, fill_value=0)[0].astype(jnp.int32)
        count = jnp.sum(chosen.astype(jnp.int32))
        live = (slot_index < count).astype(jnp.float32)
        rows = normed[owner[picks]]
        gate = jnp.dot(rows, expert_gate[expert], preferred_element_type=jnp.float32)
        up = jnp.dot(rows, expert_up[expert], preferred_element_type=jnp.float32)
        hidden = (jax.nn.silu(gate) * up).astype(jnp.bfloat16)
        down = expert_down[expert]
        result = jnp.zeros((slots, D), jnp.float32)
        for part_index in range(N_TP):
            piece = jnp.dot(hidden[:, part_index * block:(part_index + 1) * block], down[part_index * block:(part_index + 1) * block], preferred_element_type=jnp.float32)
            result = result + piece.astype(jnp.bfloat16).astype(jnp.float32)
        result = result.astype(jnp.bfloat16)
        scaled = result.astype(jnp.float32) * (weights[picks] * live)[:, None]
        return (total.at[owner[picks]].add(scaled), None)
    moe, _ = lax.scan(per_expert, jnp.zeros((TOKENS, D), jnp.float32), jnp.arange(EXPERTS, dtype=jnp.int32))
    return (mixed + moe).astype(jnp.bfloat16)
```

```python
import functools

import jax
import jax.numpy as jnp
from jax import lax
from jax.experimental import pallas as pl
from jax.experimental.pallas import tpu as pltpu
from jax.sharding import PartitionSpec as P

TOPK = 2


def with_halo(cells, sides, width):
    for axis, dim in sides:
        count = lax.axis_size(axis)
        ends = count - 1
        head = lax.slice_in_dim(cells, 0, width, axis=dim)
        tail = lax.slice_in_dim(cells, cells.shape[dim] - width, cells.shape[dim], axis=dim)
        cells = jnp.concatenate(
            [
                lax.ppermute(tail, axis, [(i, (i + 1) % count) for i in range(ends)]),
                cells,
                lax.ppermute(head, axis, [((i + 1) % count, i) for i in range(ends)]),
            ],
            axis=dim,
        )
    return cells


def on_device(
    residual,
    glu_value,
    glu_gate,
    conv_weight,
    conv_bias,
    ln_gain,
    ln_bias,
    out_weight,
    norm_gain,
    route_ids,
    route_weight,
    expert_gate,
    expert_up,
    expert_down,
):
    rows = residual.shape[0]
    width_all = out_weight.shape[0]
    gated = (glu_value.astype(jnp.float32) * jax.nn.sigmoid(glu_gate.astype(jnp.float32))).astype(
        jnp.bfloat16
    )
    reach = conv_weight.shape[0] // 2
    padded = with_halo(gated, (("sp", 0),), reach)
    taps = conv_weight.astype(jnp.float32)
    conv = jnp.zeros(gated.shape, jnp.float32) + conv_bias
    for tap in range(conv_weight.shape[0]):
        conv = conv + padded[tap : tap + rows].astype(jnp.float32) * taps[tap]
    totals = lax.psum((jnp.sum(conv, axis=1), jnp.sum(conv * conv, axis=1)), "tp")
    mean = (totals[0] / width_all)[:, None]
    var = (totals[1] / width_all)[:, None] - mean * mean
    act = jax.nn.silu((conv - mean) * lax.rsqrt(var + 1e-05) * ln_gain + ln_bias).astype(
        jnp.bfloat16
    )
    projected = jnp.dot(
        lax.all_gather(act, "tp", axis=1, tiled=True),
        out_weight,
        preferred_element_type=jnp.float32,
    )
    mixed = residual.astype(jnp.float32) + projected
    squares = lax.psum(jnp.sum(mixed * mixed, axis=1), "tp")
    normed = (mixed * lax.rsqrt(squares / width_all + 1e-06)[:, None] * norm_gain).astype(
        jnp.bfloat16
    )
    experts = lax.axis_size("sp")
    capacity = 2 * rows * TOPK // experts
    flat = route_ids.reshape(-1)
    onehot = (flat[:, None] == jnp.arange(experts, dtype=jnp.int32)[None, :]).astype(jnp.int32)
    rank = jnp.sum((jnp.cumsum(onehot, axis=0) - 1) * onehot, axis=1)
    slot_of = flat * capacity + rank
    placing = (slot_of[None, :] == jnp.arange(experts * capacity, dtype=jnp.int32)[:, None]).astype(
        jnp.bfloat16
    )
    copies = jnp.repeat(normed, TOPK, axis=0)
    outgoing = jnp.dot(placing, copies, preferred_element_type=jnp.float32).astype(jnp.bfloat16)
    outgoing = outgoing.reshape(experts, capacity, normed.shape[1])
    arrived = lax.all_to_all(outgoing, "sp", split_axis=0, concat_axis=0, tiled=True)
    arrived = lax.all_gather(
        arrived.reshape(experts * capacity, normed.shape[1]), "tp", axis=1, tiled=True
    )
    gate = jnp.dot(arrived, expert_gate[0], preferred_element_type=jnp.float32)
    up = jnp.dot(arrived, expert_up[0], preferred_element_type=jnp.float32)
    hidden = (jax.nn.silu(gate) * up).astype(jnp.bfloat16)
    partial_out = jnp.dot(hidden, expert_down[0], preferred_element_type=jnp.float32)
    summed = lax.psum_scatter(
        partial_out.astype(jnp.bfloat16), "tp", scatter_dimension=1, tiled=True
    )
    summed = summed.reshape(experts, capacity, summed.shape[1])
    returned = lax.all_to_all(summed, "sp", split_axis=0, concat_axis=0, tiled=True)
    returned = returned.reshape(experts * capacity, returned.shape[2])
    picked = lax.dot_general(
        placing, returned, (((0,), (0,)), ((), ())), preferred_element_type=jnp.float32
    )
    picked = picked.reshape(rows, TOPK, picked.shape[1])
    moe = jnp.sum(picked * route_weight[:, :, None], axis=1)
    return (mixed + moe).astype(jnp.bfloat16)


F32 = jnp.float32
BF16 = jnp.bfloat16
GROUPS = 4


def dot(a, b):
    return jnp.dot(a, b, preferred_element_type=F32)


def layer_kernel(
    nsp, ntp,
    res_ref, val_ref, gate_ref, cw_ref, cb_ref, lg_ref, lb_ref, ng_ref, ids_ref, rw_ref,
    ow_hbm, eg_hbm, eu_hbm, ed_hbm,
    out_ref,
    ow, wg, wu, wd, pad, wf, conv, mixed, halo_out, halo_in, st_out, st_in,
    act, outgoing, arr, hid, part, one, two_out, two, fin, ret,
    w_sem, halo_s, halo_r, st_s, st_r, ag_s, ag_r, zs_s, zs_r, x_s, x_r, r_s, r_r, h_s, h_r,
):
    rows, ch = res_ref.shape
    width = ow.shape[0]
    taps = cw_ref.shape[0]
    reach = taps // 2
    edge = halo_in.shape[1]
    size = nsp // GROUPS
    cap = outgoing.shape[0] // nsp
    grp = size * cap
    half = grp // 2
    me = lax.axis_index("sp")
    t = lax.axis_index("tp")
    gi, mi = me // size, me % size
    cx, cy = t % 2, t // 2
    tx = cy * 2 + 1 - cx
    ty = (1 - cy) * 2 + cx
    td = (1 - cy) * 2 + 1 - cx

    def remote(src, dst, ss, rs, **dev):
        return pltpu.make_async_remote_copy(
            src_ref=src, dst_ref=dst, send_sem=ss, recv_sem=rs,
            device_id=dev, device_id_type=pl.DeviceIdType.MESH,
        )

    barrier = pltpu.get_barrier_semaphore()
    for d in range(1, ntp):
        pl.semaphore_signal(barrier, inc=1, device_id={"tp": (t + d) % ntp},
                            device_id_type=pl.DeviceIdType.MESH)
    for d in range(1, nsp):
        pl.semaphore_signal(barrier, inc=1, device_id={"sp": (me + d) % nsp},
                            device_id_type=pl.DeviceIdType.MESH)
    loads = [
        pltpu.make_async_copy(ow_hbm, ow, w_sem.at[0]),
        pltpu.make_async_copy(eg_hbm.at[0], wg, w_sem.at[1]),
        pltpu.make_async_copy(eu_hbm.at[0], wu, w_sem.at[2]),
        pltpu.make_async_copy(ed_hbm.at[0], wd, w_sem.at[3]),
    ]
    for load in loads:
        load.start()

    gated = (val_ref[...].astype(F32) * jax.nn.sigmoid(gate_ref[...].astype(F32))).astype(BF16)
    halo_out[0] = gated[rows - edge:]
    halo_out[1] = gated[:edge]
    pad[edge:edge + rows, :] = gated.astype(F32)
    pad[0:edge, :] = jnp.zeros((edge, ch), F32)
    pad[edge + rows:, :] = jnp.zeros((edge, ch), F32)
    wf[0:taps, :] = cw_ref[...].astype(F32)
    pl.semaphore_wait(barrier, ntp + nsp - 2)
    to_right = remote(halo_out.at[0], halo_in.at[0], halo_s.at[0], halo_r.at[0], sp=(me + 1) % nsp)
    to_left = remote(halo_out.at[1], halo_in.at[1], halo_s.at[1], halo_r.at[1],
                     sp=(me + nsp - 1) % nsp)

    @pl.when(me < nsp - 1)
    def _():
        to_right.start()

    @pl.when(me > 0)
    def _():
        to_left.start()

    lane = lax.broadcasted_iota(jnp.int32, (rows, 128), 1)
    row = lax.broadcasted_iota(jnp.int32, (rows, rows), 0)
    col = lax.broadcasted_iota(jnp.int32, (rows, rows), 1)
    id0, id1 = ids_ref[:, 0:1], ids_ref[:, 1:2]
    hit0, hit1 = lane == id0, lane == id1
    named = jnp.where(hit0, 1.0, jnp.where(hit1, 1.0, 0.0)).astype(BF16)
    before = jnp.where(col < row, 1.0, 0.0).astype(BF16)
    rank = dot(before, named)
    rank0 = jnp.sum(jnp.where(hit0, rank, 0.0), axis=1, keepdims=True).astype(jnp.int32)
    rank1 = jnp.sum(jnp.where(hit1, rank, 0.0), axis=1, keepdims=True).astype(jnp.int32)
    slot = lax.broadcasted_iota(jnp.int32, (rows, nsp * cap), 1)
    pick0 = jnp.where(slot == id0 * cap + rank0, 1.0, 0.0)
    pick1 = jnp.where(slot == id1 * cap + rank1, 1.0, 0.0)
    placing = (pick0 + pick1).T.astype(BF16)
    pick0 = pick0.astype(BF16)
    pick1 = pick1.astype(BF16)

    @pl.when(me > 0)
    def _():
        to_right.wait_recv()
        pad[0:edge, :] = halo_in[0].astype(F32)

    @pl.when(me < nsp - 1)
    def _():
        to_left.wait_recv()
        pad[edge + rows:, :] = halo_in[1].astype(F32)

    for j in range(0, ch, 128):
        total = jnp.zeros((rows, 128), F32) + cb_ref[:, j:j + 128]
        for tap in range(taps):
            at = tap + edge - reach
            total = total + pad[at:at + rows, j:j + 128] * wf[tap:tap + 1, j:j + 128]
        conv[:, j:j + 128] = total

    def row_totals(which, sums):
        block = jnp.zeros((rows, 128), F32)
        for n, s in enumerate(sums):
            block = jnp.where(lane == n, s, block)
        mine = block.T[0:8, :]
        st_out[which] = mine
        copies = []
        for d in range(1, ntp):
            n = which * ntp + d
            copy = remote(st_out.at[which], st_in.at[which, d], st_s.at[n], st_r.at[n],
                          tp=(t + d) % ntp)
            copy.start()
            copies.append(copy)
        total = mine
        for d, copy in enumerate(copies):
            copy.wait_recv()
            total = total + st_in[which, d + 1]
        back = jnp.concatenate([total, jnp.zeros((rows - 8, 128), F32)], axis=0).T
        return [back[:, n:n + 1] for n in range(len(sums))], copies

    c = conv[...]
    (s1, s2), st1 = row_totals(
        0, (jnp.sum(c, axis=1, keepdims=True), jnp.sum(c * c, axis=1, keepdims=True))
    )
    mean = s1 / width
    var = s2 / width - mean * mean
    act[t] = jax.nn.silu(
        (conv[...] - mean) * lax.rsqrt(var + 1e-05) * lg_ref[...] + lb_ref[...]
    ).astype(BF16)

    mid = rows // 2
    ag = [
        remote(act.at[t], act.at[t], ag_s.at[0], ag_r.at[0], tp=tx),
        remote(act.at[t], act.at[t], ag_s.at[1], ag_r.at[1], tp=ty),
        remote(act.at[tx, pl.ds(0, mid)], act.at[tx, pl.ds(0, mid)], ag_s.at[2], ag_r.at[2], tp=ty),
        remote(act.at[ty, pl.ds(mid, mid)], act.at[ty, pl.ds(mid, mid)], ag_s.at[3], ag_r.at[3],
               tp=tx),
    ]

    def arrival(n, block):
        return remote(block, block, ag_s.at[n], ag_r.at[n], tp=tx)

    def columns(of):
        return ow[pl.ds(pl.multiple_of(of * ch, ch), ch), :]

    ag[0].start()
    ag[1].start()
    loads[0].wait()
    mixed[...] = res_ref[...].astype(F32) + dot(act[t], columns(t))
    arrival(0, act.at[tx]).wait_recv()
    ag[2].start()
    arrival(1, act.at[ty]).wait_recv()
    ag[3].start()
    mixed[...] += dot(act[tx], columns(tx)) + dot(act[ty], columns(ty))
    arrival(2, act.at[td, pl.ds(0, mid)]).wait_recv()
    arrival(3, act.at[td, pl.ds(mid, mid)]).wait_recv()
    full = mixed[...] + dot(act[td], columns(td))
    mixed[...] = full
    (sq,), st2 = row_totals(1, (jnp.sum(full * full, axis=1, keepdims=True),))
    normed = (mixed[...] * lax.rsqrt(sq / width + 1e-06) * ng_ref[...]).astype(BF16)
    outgoing[...] = dot(placing, normed).astype(BF16)

    def piece(n):
        return pl.ds(pl.multiple_of(n * cap, cap), cap)

    zs = []
    for k in range(GROUPS):
        for i in range(size):
            if k == 0 and i == 0:
                continue
            e = (gi - k + GROUPS) % GROUPS * size + (mi + i) % size
            place = k * size + mi
            copy = remote(outgoing.at[piece(e)], arr.at[t, piece(place)],
                          zs_s.at[k * size + i], zs_r.at[place], sp=e)
            copy.start()
            zs.append(copy)
    arr[t, piece(mi), :] = outgoing[piece(me), :]

    pending = []

    def send(copy):
        copy.start()
        pending.append(copy)

    def span(k):
        return pl.ds(k * grp, grp)

    def front(k):
        return pl.ds(k * grp, half)

    def rear(k):
        return pl.ds(k * grp + half, half)

    def share(k):
        for i in range(size):
            if k == 0 and i == 0:
                continue
            place = k * size + (mi + i) % size
            remote(outgoing.at[piece(0)], arr.at[t, piece(place)], zs_s.at[0], zs_r.at[place],
                   sp=me).wait_recv()
        own = arr.at[t, span(k)]
        send(remote(own, own, x_s.at[4 * k], x_r.at[4 * k], tp=tx))
        send(remote(own, own, x_s.at[4 * k + 1], x_r.at[4 * k + 1], tp=ty))

    def landed(n, block):
        remote(block, block, x_s.at[n], x_r.at[n], tp=tx).wait_recv()

    def relay(k):
        landed(4 * k, arr.at[tx, span(k)])
        block = arr.at[tx, front(k)]
        send(remote(block, block, x_s.at[4 * k + 2], x_r.at[4 * k + 2], tp=ty))
        landed(4 * k + 1, arr.at[ty, span(k)])
        block = arr.at[ty, rear(k)]
        send(remote(block, block, x_s.at[4 * k + 3], x_r.at[4 * k + 3], tp=tx))

    def gather_end(k):
        landed(4 * k + 2, arr.at[td, front(k)])
        landed(4 * k + 3, arr.at[td, rear(k)])

    inner = wg.shape[1]
    tile = min(256, inner)

    def experts(k):
        def up(n, carry):
            at = pl.ds(pl.multiple_of(n * tile, tile), tile)
            g = jnp.zeros((grp, tile), F32)
            u = jnp.zeros((grp, tile), F32)
            for b in range(ntp):
                x = arr[b, k * grp:(k + 1) * grp, :]
                g = g + dot(x, wg[b * ch:(b + 1) * ch, at])
                u = u + dot(x, wu[b * ch:(b + 1) * ch, at])
            hid[:, at] = (jax.nn.silu(g) * u).astype(BF16)
            return carry

        def down(b, carry):
            at = pl.ds(pl.multiple_of(b * ch, ch), ch)
            part[b, k * grp:(k + 1) * grp, :] = dot(hid[...], wd[:, at]).astype(BF16)
            return carry

        if k == 0:
            loads[1].wait()
            loads[2].wait()
        lax.fori_loop(0, inner // tile, up, 0)
        if k == 0:
            loads[3].wait()
        lax.fori_loop(0, ntp, down, 0)
        n = 6 * k
        first = [
            (part.at[tx, front(k)], one.at[0, front(k)], n, tx),
            (part.at[td, front(k)], one.at[1, front(k)], n + 1, tx),
            (part.at[ty, rear(k)], one.at[0, rear(k)], n + 2, ty),
            (part.at[td, rear(k)], one.at[1, rear(k)], n + 3, ty),
        ]
        for src, dst, m, to in (first[1], first[3], first[0], first[2]):
            send(remote(src, dst, r_s.at[m], r_r.at[m], tp=to))

    def summed(m, block):
        remote(block, block, r_s.at[m], r_r.at[m], tp=tx).wait_recv()

    def reduce_mid(k):
        n = 6 * k
        for m, at, to in ((n + 1, front(k), ty), (n + 3, rear(k), tx)):
            summed(m, one.at[1, at])
            two_out[at, :] = (part[to, at, :].astype(F32) + one[1, at, :].astype(F32)).astype(BF16)
            m2 = n + 4 + (m - n) // 2
            send(remote(two_out.at[at], two.at[at], r_s.at[m2], r_r.at[m2], tp=to))

    def reduce_end(k):
        n = 6 * k
        summed(n, one.at[0, front(k)])
        summed(n + 2, one.at[0, rear(k)])
        summed(n + 4, two.at[front(k)])
        summed(n + 5, two.at[rear(k)])
        at = span(k)
        fin[at, :] = (
            part[t, at, :].astype(F32) + one[0, at, :].astype(F32) + two[at, :].astype(F32)
        ).astype(BF16)
        for i in range(size):
            if k == 0 and i == 0:
                ret[piece(me), :] = fin[piece(mi), :]
                continue
            who = (mi + i) % size
            home = (gi + k) % GROUPS * size + who
            send(remote(fin.at[piece(k * size + who)], ret.at[piece(me)],
                        h_s.at[k * size + i], h_r.at[me], sp=home))

    for k in range(GROUPS):
        if k == 0:
            share(0)
            share(1)
        relay(k)
        if 0 < k < GROUPS - 1:
            share(k + 1)
        gather_end(k)
        experts(k)
        if k >= 1:
            reduce_mid(k - 1)
        if k >= 2:
            reduce_end(k - 2)
    reduce_end(GROUPS - 2)
    reduce_mid(GROUPS - 1)
    reduce_end(GROUPS - 1)

    for d in range(1, nsp):
        e = (me + d) % nsp
        remote(fin.at[piece(0)], ret.at[piece(e)], h_s.at[0], h_r.at[e], sp=me).wait_recv()
    back = ret[...]
    moe = dot(pick0, back) * rw_ref[:, 0:1] + dot(pick1, back) * rw_ref[:, 1:2]
    out_ref[...] = (mixed[...] + moe).astype(out_ref.dtype)

    @pl.when(me < nsp - 1)
    def _():
        to_right.wait_send()

    @pl.when(me > 0)
    def _():
        to_left.wait_send()

    for copy in st1 + st2 + ag + zs + pending:
        copy.wait_send()


def fused(nsp, ntp, *args):
    (residual, glu_value, glu_gate, conv_weight, conv_bias, ln_gain, ln_bias, out_weight,
     norm_gain, route_ids, route_weight, expert_gate, expert_up, expert_down) = args
    rows, ch = residual.shape
    width = out_weight.shape[0]
    inner = expert_gate.shape[2]
    cap = 2 * rows * TOPK // nsp
    slots = nsp * cap
    grp = slots // GROUPS
    edge = -(-(conv_weight.shape[0] // 2) // 16) * 16
    vmem = pl.BlockSpec(memory_space=pltpu.VMEM)
    hbm = pl.BlockSpec(memory_space=pl.ANY)
    dma = lambda n: pltpu.SemaphoreType.DMA((n,))
    return pl.pallas_call(
        functools.partial(layer_kernel, nsp, ntp),
        out_shape=jax.ShapeDtypeStruct((rows, ch), residual.dtype),
        in_specs=[vmem] * 10 + [hbm] * 4,
        out_specs=vmem,
        scratch_shapes=[
            pltpu.VMEM((width, ch), BF16),
            pltpu.VMEM((width, inner), BF16),
            pltpu.VMEM((width, inner), BF16),
            pltpu.VMEM((inner, width), BF16),
            pltpu.VMEM((rows + 2 * edge, ch), F32),
            pltpu.VMEM((-(-conv_weight.shape[0] // 8) * 8, ch), F32),
            pltpu.VMEM((rows, ch), F32),
            pltpu.VMEM((rows, ch), F32),
            pltpu.VMEM((2, edge, ch), BF16),
            pltpu.VMEM((2, edge, ch), BF16),
            pltpu.VMEM((2, 8, 128), F32),
            pltpu.VMEM((2, ntp, 8, 128), F32),
            pltpu.VMEM((ntp, rows, ch), BF16),
            pltpu.VMEM((slots, ch), BF16),
            pltpu.VMEM((ntp, slots, ch), BF16),
            pltpu.VMEM((grp, inner), BF16),
            pltpu.VMEM((ntp, slots, ch), BF16),
            pltpu.VMEM((2, slots, ch), BF16),
            pltpu.VMEM((slots, ch), BF16),
            pltpu.VMEM((slots, ch), BF16),
            pltpu.VMEM((slots, ch), BF16),
            pltpu.VMEM((slots, ch), BF16),
            dma(4), dma(2), dma(2), dma(2 * ntp), dma(2 * ntp), dma(4), dma(4),
            dma(nsp), dma(nsp), dma(4 * GROUPS), dma(4 * GROUPS), dma(6 * GROUPS),
            dma(6 * GROUPS), dma(nsp), dma(nsp),
        ],
        compiler_params=pltpu.CompilerParams(
            collective_id=0, has_side_effects=True, vmem_limit_bytes=52 * 1024 * 1024
        ),
    )(residual, glu_value, glu_gate, conv_weight, conv_bias.reshape(1, ch), ln_gain.reshape(1, ch),
      ln_bias.reshape(1, ch), norm_gain.reshape(1, ch), route_ids, route_weight,
      out_weight, expert_gate, expert_up, expert_down)


def solution(mesh):
    in_specs = (
        P("sp", "tp"),
        P("sp", "tp"),
        P("sp", "tp"),
        P(None, "tp"),
        P("tp"),
        P("tp"),
        P("tp"),
        P(None, "tp"),
        P("tp"),
        P("sp", None),
        P("sp", None),
        P("sp", None, "tp"),
        P("sp", None, "tp"),
        P("sp", "tp", None),
    )
    out_specs = P("sp", "tp")
    nsp, ntp = mesh.shape["sp"], mesh.shape["tp"]
    body = on_device
    if ntp == 4 and nsp % GROUPS == 0:
        body = functools.partial(fused, nsp, ntp)
    return jax.shard_map(
        body, mesh=mesh, in_specs=in_specs, out_specs=out_specs, check_vma=False
    )
```

```python
import functools

import jax
import jax.numpy as jnp
from jax import lax
from jax.experimental import pallas as pl
from jax.experimental.pallas import tpu as pltpu
from jax.sharding import PartitionSpec as P

TOPK = 2


def with_halo(cells, sides, width):
    for axis, dim in sides:
        count = lax.axis_size(axis)
        ends = count - 1
        head = lax.slice_in_dim(cells, 0, width, axis=dim)
        tail = lax.slice_in_dim(cells, cells.shape[dim] - width, cells.shape[dim], axis=dim)
        cells = jnp.concatenate(
            [
                lax.ppermute(tail, axis, [(i, (i + 1) % count) for i in range(ends)]),
                cells,
                lax.ppermute(head, axis, [((i + 1) % count, i) for i in range(ends)]),
            ],
            axis=dim,
        )
    return cells


def on_device(
    residual,
    glu_value,
    glu_gate,
    conv_weight,
    conv_bias,
    ln_gain,
    ln_bias,
    out_weight,
    norm_gain,
    route_ids,
    route_weight,
    expert_gate,
    expert_up,
    expert_down,
):
    rows = residual.shape[0]
    width_all = out_weight.shape[0]
    gated = (glu_value.astype(jnp.float32) * jax.nn.sigmoid(glu_gate.astype(jnp.float32))).astype(
        jnp.bfloat16
    )
    reach = conv_weight.shape[0] // 2
    padded = with_halo(gated, (("sp", 0),), reach)
    taps = conv_weight.astype(jnp.float32)
    conv = jnp.zeros(gated.shape, jnp.float32) + conv_bias
    for tap in range(conv_weight.shape[0]):
        conv = conv + padded[tap : tap + rows].astype(jnp.float32) * taps[tap]
    totals = lax.psum((jnp.sum(conv, axis=1), jnp.sum(conv * conv, axis=1)), "tp")
    mean = (totals[0] / width_all)[:, None]
    var = (totals[1] / width_all)[:, None] - mean * mean
    act = jax.nn.silu((conv - mean) * lax.rsqrt(var + 1e-05) * ln_gain + ln_bias).astype(
        jnp.bfloat16
    )
    projected = jnp.dot(
        lax.all_gather(act, "tp", axis=1, tiled=True),
        out_weight,
        preferred_element_type=jnp.float32,
    )
    mixed = residual.astype(jnp.float32) + projected
    squares = lax.psum(jnp.sum(mixed * mixed, axis=1), "tp")
    normed = (mixed * lax.rsqrt(squares / width_all + 1e-06)[:, None] * norm_gain).astype(
        jnp.bfloat16
    )
    experts = lax.axis_size("sp")
    capacity = 2 * rows * TOPK // experts
    flat = route_ids.reshape(-1)
    onehot = (flat[:, None] == jnp.arange(experts, dtype=jnp.int32)[None, :]).astype(jnp.int32)
    rank = jnp.sum((jnp.cumsum(onehot, axis=0) - 1) * onehot, axis=1)
    slot_of = flat * capacity + rank
    placing = (slot_of[None, :] == jnp.arange(experts * capacity, dtype=jnp.int32)[:, None]).astype(
        jnp.bfloat16
    )
    copies = jnp.repeat(normed, TOPK, axis=0)
    outgoing = jnp.dot(placing, copies, preferred_element_type=jnp.float32).astype(jnp.bfloat16)
    outgoing = outgoing.reshape(experts, capacity, normed.shape[1])
    arrived = lax.all_to_all(outgoing, "sp", split_axis=0, concat_axis=0, tiled=True)
    arrived = lax.all_gather(
        arrived.reshape(experts * capacity, normed.shape[1]), "tp", axis=1, tiled=True
    )
    gate = jnp.dot(arrived, expert_gate[0], preferred_element_type=jnp.float32)
    up = jnp.dot(arrived, expert_up[0], preferred_element_type=jnp.float32)
    hidden = (jax.nn.silu(gate) * up).astype(jnp.bfloat16)
    partial_out = jnp.dot(hidden, expert_down[0], preferred_element_type=jnp.float32)
    summed = lax.psum_scatter(
        partial_out.astype(jnp.bfloat16), "tp", scatter_dimension=1, tiled=True
    )
    summed = summed.reshape(experts, capacity, summed.shape[1])
    returned = lax.all_to_all(summed, "sp", split_axis=0, concat_axis=0, tiled=True)
    returned = returned.reshape(experts * capacity, returned.shape[2])
    picked = lax.dot_general(
        placing, returned, (((0,), (0,)), ((), ())), preferred_element_type=jnp.float32
    )
    picked = picked.reshape(rows, TOPK, picked.shape[1])
    moe = jnp.sum(picked * route_weight[:, :, None], axis=1)
    return (mixed + moe).astype(jnp.bfloat16)


F32 = jnp.float32
BF16 = jnp.bfloat16
GROUPS = 4


def dot(a, b):
    return jnp.dot(a, b, preferred_element_type=F32)


def layer_kernel(
    nsp, ntp,
    res_hbm, val_hbm, gate_hbm, cw_hbm, cb_hbm, lg_hbm, lb_hbm, ng_hbm, ids_hbm, rw_hbm,
    ow_hbm, eg_hbm, eu_hbm, ed_hbm,
    out_ref,
    res_ref, val_ref, gate_ref, cw_ref, cb_ref, lg_ref, lb_ref, ng_ref, ids_ref, rw_ref,
    ow, wg, wu, wd, pad, wf, conv, mixed, halo_out, halo_in, st_out, st_in,
    act, outgoing, arr, hid, part, one, two_out, two, fin, ret,
    w_sem, halo_s, halo_r, st_s, st_r, ag_s, ag_r, zs_s, zs_r, x_s, x_r, r_s, r_r, h_s, h_r,
):
    rows, ch = res_ref.shape
    width = ow.shape[0]
    taps = cw_ref.shape[0]
    reach = taps // 2
    edge = halo_in.shape[1]
    size = nsp // GROUPS
    cap = outgoing.shape[0] // nsp
    grp = size * cap
    half = grp // 2
    me = lax.axis_index("sp")
    t = lax.axis_index("tp")
    gi, mi = me // size, me % size
    cx, cy = t % 2, t // 2
    tx = cy * 2 + 1 - cx
    ty = (1 - cy) * 2 + cx
    td = (1 - cy) * 2 + 1 - cx

    def remote(src, dst, ss, rs, **dev):
        return pltpu.make_async_remote_copy(
            src_ref=src, dst_ref=dst, send_sem=ss, recv_sem=rs,
            device_id=dev, device_id_type=pl.DeviceIdType.MESH,
        )

    smalls = [
        (val_hbm, val_ref), (gate_hbm, gate_ref), (cw_hbm, cw_ref), (cb_hbm, cb_ref),
        (ids_hbm, ids_ref), (lg_hbm, lg_ref), (lb_hbm, lb_ref), (res_hbm, res_ref),
        (ng_hbm, ng_ref), (rw_hbm, rw_ref),
    ]
    staged = [pltpu.make_async_copy(a, b, w_sem.at[4 + n]) for n, (a, b) in enumerate(smalls)]
    for load in staged:
        load.start()
    barrier = pltpu.get_barrier_semaphore()
    for d in range(1, ntp):
        pl.semaphore_signal(barrier, inc=1, device_id={"tp": (t + d) % ntp},
                            device_id_type=pl.DeviceIdType.MESH)
    for d in range(1, nsp):
        pl.semaphore_signal(barrier, inc=1, device_id={"sp": (me + d) % nsp},
                            device_id_type=pl.DeviceIdType.MESH)
    loads = [
        pltpu.make_async_copy(ow_hbm, ow, w_sem.at[0]),
        pltpu.make_async_copy(eg_hbm.at[0], wg, w_sem.at[1]),
        pltpu.make_async_copy(eu_hbm.at[0], wu, w_sem.at[2]),
        pltpu.make_async_copy(ed_hbm.at[0], wd, w_sem.at[3]),
    ]
    for load in loads:
        load.start()

    staged[0].wait()
    staged[1].wait()
    gated = (val_ref[...].astype(F32) * jax.nn.sigmoid(gate_ref[...].astype(F32))).astype(BF16)
    halo_out[0] = gated[rows - edge:]
    halo_out[1] = gated[:edge]
    pad[edge:edge + rows, :] = gated.astype(F32)
    pad[0:edge, :] = jnp.zeros((edge, ch), F32)
    pad[edge + rows:, :] = jnp.zeros((edge, ch), F32)
    staged[2].wait()
    wf[0:taps, :] = cw_ref[...].astype(F32)
    pl.semaphore_wait(barrier, ntp + nsp - 2)
    to_right = remote(halo_out.at[0], halo_in.at[0], halo_s.at[0], halo_r.at[0], sp=(me + 1) % nsp)
    to_left = remote(halo_out.at[1], halo_in.at[1], halo_s.at[1], halo_r.at[1],
                     sp=(me + nsp - 1) % nsp)

    @pl.when(me < nsp - 1)
    def _():
        to_right.start()

    @pl.when(me > 0)
    def _():
        to_left.start()

    lane = lax.broadcasted_iota(jnp.int32, (rows, 128), 1)
    row = lax.broadcasted_iota(jnp.int32, (rows, rows), 0)
    col = lax.broadcasted_iota(jnp.int32, (rows, rows), 1)
    for load in staged[3:]:
        load.wait()
    topk = ids_ref.shape[0]

    def upright(pair):
        return jnp.concatenate([pair, jnp.zeros((128 - topk, rows), F32)], axis=0).T

    ids = upright(ids_ref[...].astype(F32)).astype(jnp.int32)
    id0, id1 = ids[:, 0:1], ids[:, 1:2]
    weights = upright(rw_ref[...])
    hit0, hit1 = lane == id0, lane == id1
    named = jnp.where(hit0, 1.0, jnp.where(hit1, 1.0, 0.0)).astype(BF16)
    before = jnp.where(col < row, 1.0, 0.0).astype(BF16)
    rank = dot(before, named)
    rank0 = jnp.sum(jnp.where(hit0, rank, 0.0), axis=1, keepdims=True).astype(jnp.int32)
    rank1 = jnp.sum(jnp.where(hit1, rank, 0.0), axis=1, keepdims=True).astype(jnp.int32)
    slot = lax.broadcasted_iota(jnp.int32, (rows, nsp * cap), 1)
    pick0 = jnp.where(slot == id0 * cap + rank0, 1.0, 0.0)
    pick1 = jnp.where(slot == id1 * cap + rank1, 1.0, 0.0)
    placing = (pick0 + pick1).T.astype(BF16)
    pick0 = pick0.astype(BF16)
    pick1 = pick1.astype(BF16)

    @pl.when(me > 0)
    def _():
        to_right.wait_recv()
        pad[0:edge, :] = halo_in[0].astype(F32)

    @pl.when(me < nsp - 1)
    def _():
        to_left.wait_recv()
        pad[edge + rows:, :] = halo_in[1].astype(F32)

    for j in range(0, ch, 128):
        total = jnp.zeros((rows, 128), F32) + cb_ref[:, j:j + 128]
        for tap in range(taps):
            at = tap + edge - reach
            total = total + pad[at:at + rows, j:j + 128] * wf[tap:tap + 1, j:j + 128]
        conv[:, j:j + 128] = total

    def row_totals(which, sums):
        block = jnp.zeros((rows, 128), F32)
        for n, s in enumerate(sums):
            block = jnp.where(lane == n, s, block)
        mine = block.T[0:8, :]
        st_out[which] = mine
        copies = []
        for d in range(1, ntp):
            n = which * ntp + d
            copy = remote(st_out.at[which], st_in.at[which, d], st_s.at[n], st_r.at[n],
                          tp=(t + d) % ntp)
            copy.start()
            copies.append(copy)
        total = mine
        for d, copy in enumerate(copies):
            copy.wait_recv()
            total = total + st_in[which, d + 1]
        back = jnp.concatenate([total, jnp.zeros((rows - 8, 128), F32)], axis=0).T
        return [back[:, n:n + 1] for n in range(len(sums))], copies

    c = conv[...]
    (s1, s2), st1 = row_totals(
        0, (jnp.sum(c, axis=1, keepdims=True), jnp.sum(c * c, axis=1, keepdims=True))
    )
    mean = s1 / width
    var = s2 / width - mean * mean
    act[t] = jax.nn.silu(
        (conv[...] - mean) * lax.rsqrt(var + 1e-05) * lg_ref[...] + lb_ref[...]
    ).astype(BF16)

    mid = rows // 2
    low, high = pl.ds(0, mid), pl.ds(mid, mid)
    ag = [
        remote(act.at[of, at], act.at[of, at], ag_s.at[n], ag_r.at[n], tp=to)
        for n, (of, at, to) in enumerate((
            (t, low, tx), (t, high, ty), (t, high, tx), (t, low, ty), (tx, low, ty), (ty, high, tx),
        ))
    ]

    def arrival(n, block):
        return remote(block, block, ag_s.at[n], ag_r.at[n], tp=tx)

    def columns(of):
        return ow[pl.ds(pl.multiple_of(of * ch, ch), ch), :]

    for n in range(4):
        ag[n].start()
    loads[0].wait()
    mixed[...] = res_ref[...].astype(F32) + dot(act[t], columns(t))
    arrival(0, act.at[tx, low]).wait_recv()
    ag[4].start()
    arrival(1, act.at[ty, high]).wait_recv()
    ag[5].start()
    arrival(2, act.at[tx, high]).wait_recv()
    arrival(3, act.at[ty, low]).wait_recv()
    mixed[...] += dot(act[tx], columns(tx)) + dot(act[ty], columns(ty))
    arrival(4, act.at[td, low]).wait_recv()
    arrival(5, act.at[td, high]).wait_recv()
    full = mixed[...] + dot(act[td], columns(td))
    mixed[...] = full
    (sq,), st2 = row_totals(1, (jnp.sum(full * full, axis=1, keepdims=True),))
    normed = (mixed[...] * lax.rsqrt(sq / width + 1e-06) * ng_ref[...]).astype(BF16)
    outgoing[...] = dot(placing, normed).astype(BF16)

    def piece(n):
        return pl.ds(pl.multiple_of(n * cap, cap), cap)

    zs = []
    for k in range(GROUPS):
        for i in range(size):
            if k == 0 and i == 0:
                continue
            e = (gi - k + GROUPS) % GROUPS * size + (mi + i) % size
            place = k * size + mi
            copy = remote(outgoing.at[piece(e)], arr.at[t, piece(place)],
                          zs_s.at[k * size + i], zs_r.at[place], sp=e)
            copy.start()
            zs.append(copy)
    arr[t, piece(mi), :] = outgoing[piece(me), :]

    pending = []

    def send(copy):
        copy.start()
        pending.append(copy)

    def span(k):
        return pl.ds(k * grp, grp)

    def front(k):
        return pl.ds(k * grp, half)

    def rear(k):
        return pl.ds(k * grp + half, half)

    def share(k):
        for i in range(size):
            if k == 0 and i == 0:
                continue
            place = k * size + (mi + i) % size
            remote(outgoing.at[piece(0)], arr.at[t, piece(place)], zs_s.at[0], zs_r.at[place],
                   sp=me).wait_recv()
        pass_on(k, 0, t, front(k), tx)
        pass_on(k, 1, t, rear(k), ty)
        pass_on(k, 2, t, rear(k), tx)
        pass_on(k, 3, t, front(k), ty)

    def pass_on(k, n, of, at, to):
        block = arr.at[of, at]
        send(remote(block, block, x_s.at[6 * k + n], x_r.at[6 * k + n], tp=to))

    def landed(k, n, of, at):
        block = arr.at[of, at]
        remote(block, block, x_s.at[6 * k + n], x_r.at[6 * k + n], tp=tx).wait_recv()

    def relay(k):
        landed(k, 0, tx, front(k))
        pass_on(k, 4, tx, front(k), ty)
        landed(k, 1, ty, rear(k))
        pass_on(k, 5, ty, rear(k), tx)

    def gather_end(k):
        landed(k, 2, tx, rear(k))
        landed(k, 3, ty, front(k))
        landed(k, 4, td, front(k))
        landed(k, 5, td, rear(k))

    inner = wg.shape[1]
    tile = min(256, inner)

    def expert_up(k):
        def up(n, carry):
            at = pl.ds(pl.multiple_of(n * tile, tile), tile)
            g = jnp.zeros((grp, tile), F32)
            u = jnp.zeros((grp, tile), F32)
            for b in range(ntp):
                x = arr[b, k * grp:(k + 1) * grp, :]
                g = g + dot(x, wg[b * ch:(b + 1) * ch, at])
                u = u + dot(x, wu[b * ch:(b + 1) * ch, at])
            hid[:, at] = (jax.nn.silu(g) * u).astype(BF16)
            return carry

        if k == 0:
            loads[1].wait()
            loads[2].wait()
        lax.fori_loop(0, inner // tile, up, 0)

    def expert_down(k):
        def down(b, carry):
            at = pl.ds(pl.multiple_of(b * ch, ch), ch)
            part[b, k * grp:(k + 1) * grp, :] = dot(hid[...], wd[:, at]).astype(BF16)
            return carry

        if k == 0:
            loads[3].wait()
        lax.fori_loop(0, ntp, down, 0)
        n = 6 * k
        first = [
            (part.at[tx, front(k)], one.at[0, front(k)], n, tx),
            (part.at[td, front(k)], one.at[1, front(k)], n + 1, tx),
            (part.at[ty, rear(k)], one.at[0, rear(k)], n + 2, ty),
            (part.at[td, rear(k)], one.at[1, rear(k)], n + 3, ty),
        ]
        for src, dst, m, to in (first[1], first[3], first[0], first[2]):
            send(remote(src, dst, r_s.at[m], r_r.at[m], tp=to))

    def summed(m, block):
        remote(block, block, r_s.at[m], r_r.at[m], tp=tx).wait_recv()

    def reduce_mid(k):
        n = 6 * k
        for m, at, to in ((n + 1, front(k), ty), (n + 3, rear(k), tx)):
            summed(m, one.at[1, at])
            two_out[at, :] = (part[to, at, :].astype(F32) + one[1, at, :].astype(F32)).astype(BF16)
            m2 = n + 4 + (m - n) // 2
            send(remote(two_out.at[at], two.at[at], r_s.at[m2], r_r.at[m2], tp=to))

    def reduce_end(k):
        n = 6 * k
        summed(n, one.at[0, front(k)])
        summed(n + 2, one.at[0, rear(k)])
        summed(n + 4, two.at[front(k)])
        summed(n + 5, two.at[rear(k)])
        at = span(k)
        fin[at, :] = (
            part[t, at, :].astype(F32) + one[0, at, :].astype(F32) + two[at, :].astype(F32)
        ).astype(BF16)
        for i in range(size):
            if k == 0 and i == 0:
                ret[piece(me), :] = fin[piece(mi), :]
                continue
            who = (mi + i) % size
            home = (gi + k) % GROUPS * size + who
            send(remote(fin.at[piece(k * size + who)], ret.at[piece(me)],
                        h_s.at[k * size + i], h_r.at[me], sp=home))

    order = [(share, 0), (relay, 0), (share, 1)]
    for k in range(GROUPS):
        order += [(gather_end, k), (expert_up, k)]
        if k >= 1:
            order += [(reduce_mid, k - 1)]
        if k + 1 < GROUPS:
            order += [(relay, k + 1)]
        order += [(expert_down, k)]
        if k + 2 < GROUPS:
            order += [(share, k + 2)]
        if k >= 1:
            order += [(reduce_end, k - 1)]
    order += [(reduce_mid, GROUPS - 1), (reduce_end, GROUPS - 1)]
    for step, k in order:
        step(k)

    for d in range(1, nsp):
        e = (me + d) % nsp
        remote(fin.at[piece(0)], ret.at[piece(e)], h_s.at[0], h_r.at[e], sp=me).wait_recv()
    back = ret[...]
    moe = dot(pick0, back) * weights[:, 0:1] + dot(pick1, back) * weights[:, 1:2]
    out_ref[...] = (mixed[...] + moe).astype(out_ref.dtype)

    @pl.when(me < nsp - 1)
    def _():
        to_right.wait_send()

    @pl.when(me > 0)
    def _():
        to_left.wait_send()

    for copy in st1 + st2 + ag + zs + pending:
        copy.wait_send()


def fused(nsp, ntp, *args):
    (residual, glu_value, glu_gate, conv_weight, conv_bias, ln_gain, ln_bias, out_weight,
     norm_gain, route_ids, route_weight, expert_gate, expert_up, expert_down) = args
    rows, ch = residual.shape
    width = out_weight.shape[0]
    inner = expert_gate.shape[2]
    cap = 2 * rows * TOPK // nsp
    slots = nsp * cap
    grp = slots // GROUPS
    edge = -(-(conv_weight.shape[0] // 2) // 16) * 16
    small = [residual, glu_value, glu_gate, conv_weight]
    small += [a.reshape(1, ch) for a in (conv_bias, ln_gain, ln_bias, norm_gain)]
    small += [route_ids.T, route_weight.T]
    vmem = pl.BlockSpec(memory_space=pltpu.VMEM)
    hbm = pl.BlockSpec(memory_space=pl.ANY)
    dma = lambda n: pltpu.SemaphoreType.DMA((n,))
    return pl.pallas_call(
        functools.partial(layer_kernel, nsp, ntp),
        out_shape=jax.ShapeDtypeStruct((rows, ch), residual.dtype),
        in_specs=[hbm] * 14,
        out_specs=vmem,
        scratch_shapes=[pltpu.VMEM(a.shape, a.dtype) for a in small] + [
            pltpu.VMEM((width, ch), BF16),
            pltpu.VMEM((width, inner), BF16),
            pltpu.VMEM((width, inner), BF16),
            pltpu.VMEM((inner, width), BF16),
            pltpu.VMEM((rows + 2 * edge, ch), F32),
            pltpu.VMEM((-(-conv_weight.shape[0] // 8) * 8, ch), F32),
            pltpu.VMEM((rows, ch), F32),
            pltpu.VMEM((rows, ch), F32),
            pltpu.VMEM((2, edge, ch), BF16),
            pltpu.VMEM((2, edge, ch), BF16),
            pltpu.VMEM((2, 8, 128), F32),
            pltpu.VMEM((2, ntp, 8, 128), F32),
            pltpu.VMEM((ntp, rows, ch), BF16),
            pltpu.VMEM((slots, ch), BF16),
            pltpu.VMEM((ntp, slots, ch), BF16),
            pltpu.VMEM((grp, inner), BF16),
            pltpu.VMEM((ntp, slots, ch), BF16),
            pltpu.VMEM((2, slots, ch), BF16),
            pltpu.VMEM((slots, ch), BF16),
            pltpu.VMEM((slots, ch), BF16),
            pltpu.VMEM((slots, ch), BF16),
            pltpu.VMEM((slots, ch), BF16),
            dma(14), dma(2), dma(2), dma(2 * ntp), dma(2 * ntp), dma(6), dma(6),
            dma(nsp), dma(nsp), dma(6 * GROUPS), dma(6 * GROUPS), dma(6 * GROUPS),
            dma(6 * GROUPS), dma(nsp), dma(nsp),
        ],
        compiler_params=pltpu.CompilerParams(
            collective_id=0, has_side_effects=True, vmem_limit_bytes=67043328
        ),
    )(*small, out_weight, expert_gate, expert_up, expert_down)


def solution(mesh):
    in_specs = (
        P("sp", "tp"),
        P("sp", "tp"),
        P("sp", "tp"),
        P(None, "tp"),
        P("tp"),
        P("tp"),
        P("tp"),
        P(None, "tp"),
        P("tp"),
        P("sp", None),
        P("sp", None),
        P("sp", None, "tp"),
        P("sp", None, "tp"),
        P("sp", "tp", None),
    )
    out_specs = P("sp", "tp")
    nsp, ntp = mesh.shape["sp"], mesh.shape["tp"]
    body = on_device
    if ntp == 4 and nsp % GROUPS == 0:
        body = functools.partial(fused, nsp, ntp)
    return jax.shard_map(
        body, mesh=mesh, in_specs=in_specs, out_specs=out_specs, check_vma=False
    )
```
